32 devices in a mesh: sp: 8 (over z, x), tp: 4 (over y, core).
Axes of the slice: x: 2, y: 2, z: 4, core: 2. Of those that a mesh axis runs over, the one named last changes fastest.
Arguments:
- resid: bfloat16 [3072, 2048], P('sp'), may hold values from -6 to 6
- cotangent: bfloat16 [3072, 2048], P('sp'), may hold values from -0.59765625 to 0.59765625
- routes: int32 [3072, 2], P('sp'), may hold values from 0 to 7, all different within a row; in each aligned block of 384 rows (0 to 383, 384 to 767, ...) at most 192 rows name the same one
- route_weight: float32 [3072, 2], P('sp'), may hold values from 0.3 to 2.2
- w_gate: bfloat16 [8, 2048, 1024], P('sp', None, 'tp'), may hold values from -0.125 to 0.125
- w_up: bfloat16 [8, 2048, 1024], P('sp', None, 'tp'), may hold values from -0.125 to 0.125
- w_down: bfloat16 [8, 1024, 2048], P('sp', 'tp'), may hold values from -0.1875 to 0.1875
- out_proj: bfloat16 [2048, 2816], P(None, 'tp'), may hold values from -0.109375 to 0.109375
- gate_pre: bfloat16 [3072, 2816], P('sp', 'tp'), may hold values from -8 to 8
- log_decay: float32 [3072, 2816], P('sp', 'tp'), may hold values from -1 to 0
- state_before: float32 [3072, 2816], P('sp', 'tp'), may hold values from -6 to 6
- step_input: bfloat16 [3072, 2816], P('sp', 'tp'), may hold values from -6 to 6
Outputs:
- grad_gate: float32 [8, 2048, 1024], P('sp', None, 'tp')
- grad_up: float32 [8, 2048, 1024], P('sp', None, 'tp')
- grad_down: float32 [8, 1024, 2048], P('sp', 'tp')
- grad_proj: float32 [2048, 2816], P('sp', 'tp')
- grad_gate_pre: bfloat16 [3072, 2816], P('sp', 'tp')
- grad_step_input: float32 [3072, 2816], P('sp', 'tp')
- grad_log_decay: float32 [3072, 2816], P('sp', 'tp')
The draws below stay inside these ranges and needn't reach their ends.
Inputs may be any that keep to these rules, and one draw needn't show every extreme that they name: `routes`: each row names 2 different experts. In the rows of one device no expert is named more than 192 times; some expert is named exactly 192 times in the rows of some devices.
All inputs are finite; a program needn't handle non-finite values.
Results may differ from the reference program's by a relative error of at most 0.02.
Values may be sent and summed in bfloat16 or wider, within the bound.
A program may use at most 128 MiB of HBM per device.

```python
import math
import jax
import jax.numpy as jnp
import numpy as np
from jax import lax

D = 2048
HEADS = 32
HEAD_DIM = 88
FE = 1024
TOP = 2
TOK_DEV = 384
STATE_CHANNELS = 2816
SEQUENCE_TOKENS = 3072
EXPERTS = 8
CAP = 192
N_SP = 8
N_TP = 4


def draw_log_decay(key, part):
    random_subkeys = jax.random.split(jax.random.fold_in(key, 17), 7)
    head_fast_prob = 0.5
    is_fast = jax.random.bernoulli(random_subkeys[0], head_fast_prob, (HEADS,))
    is_fast = jnp.repeat(is_fast, HEAD_DIM)
    slow_rate = jnp.exp(jax.random.uniform(random_subkeys[1], (STATE_CHANNELS,), jnp.float32, -0.69, 0.0)) * (0.15 / SEQUENCE_TOKENS)
    fast_rate = jax.random.uniform(random_subkeys[2], (STATE_CHANNELS,), jnp.float32, 1.0 / 50.0, 1.0 / 30.0)
    decay_rates = jnp.where(is_fast, fast_rate, slow_rate)
    jagged_level = jnp.exp(jax.random.uniform(random_subkeys[3], (SEQUENCE_TOKENS, STATE_CHANNELS), jnp.float32, -0.7, 0.7))
    block_multiplier = jnp.exp(jax.random.uniform(random_subkeys[4], (SEQUENCE_TOKENS // TOK_DEV, 1), jnp.float32, -0.69, 0.69))
    block_multiplier = jnp.repeat(block_multiplier, TOK_DEV, axis=0)
    spike_location = jax.random.randint(random_subkeys[5], (3,), 0, SEQUENCE_TOKENS)
    token_position = jnp.arange(SEQUENCE_TOKENS, dtype=jnp.int32)
    spike_flag = jnp.any(token_position[:, None] == spike_location[None, :], axis=1)
    spike_penalty = jax.random.uniform(random_subkeys[6], (SEQUENCE_TOKENS, STATE_CHANNELS), jnp.float32, 0.22, 0.69)
    return -(decay_rates[None, :] * jagged_level * block_multiplier) - jnp.where(spike_flag[:, None], spike_penalty, 0.0)


def with_spikes(drawn, own_key, source, target, shards_of, factor):
    def block_of(axis_at):
        return (jnp.arange(drawn.shape[axis_at]) // (drawn.shape[axis_at] // shards_of)).reshape((-1,) + (1,) * (drawn.ndim - 1 - axis_at))

    one_side = jax.random.permutation(own_key, shards_of)[block_of(target)]
    far = (block_of(target) + shards_of // 2) % shards_of
    return jnp.where((block_of(source) == one_side) | (block_of(source) == far), factor * drawn, drawn)


def steps_of(stream_key, extent, cuts, least, high):
    level = 1.0
    for dim, blocks in cuts:
        heights = jax.random.uniform(jax.random.fold_in(jax.random.fold_in(stream_key, 6), dim), (blocks,), jnp.float32, least / len(cuts), high / len(cuts))
        level = level * jnp.repeat(jnp.exp(heights), extent[dim] // blocks).reshape((-1,) + (1,) * (len(extent) - 1 - dim))
    return level


def shared_out(key, own, number, rows, number_of, top, bound, skew):
    order = jax.random.permutation(key, number_of)
    crowded, usual = portions_of(number_of, rows * top, bound, skew, True), portions_of(number_of, rows * top, bound, skew, False)
    places = jnp.arange(number_of)

    def named(tallies, turn):
        used = int((tallies > 0).sum())
        fixed = max(1, used // 4)
        moved = fixed + (places - fixed + turn * (used - fixed)) % max(1, number_of - fixed)
        return jnp.zeros((number_of,), jnp.int32).at[order[jnp.where(places < fixed, places, moved)]].set(jnp.asarray(tallies, jnp.int32))

    tallies = jnp.where(number % 4 == 0, named(crowded, number // 4), named(usual, number - number // 4 - 1))
    mixed = jax.random.permutation(jax.random.fold_in(own, 3), number_of)
    donor, taker = mixed[0:number_of // 2 * 2:2], mixed[1:number_of // 2 * 2:2]
    margin = jnp.minimum(tallies[donor] - 1, bound - tallies[taker]) // 2
    margin = jnp.where((donor == order[0]) | (taker == order[0]) | (tallies[taker] == 0), 0, jnp.maximum(margin, 0))
    moved = jax.random.randint(jax.random.fold_in(own, 4), (number_of // 2,), 0, 1 << 20) % (margin + 1)
    tallies = tallies.at[donor].add(-moved).at[taker].add(moved)
    items = jnp.searchsorted(jnp.cumsum(tallies), jnp.arange(rows * top), side="right").astype(jnp.int32)
    grid = items.reshape(top, rows).T
    grid = grid[jax.random.permutation(jax.random.fold_in(own, 1), rows)]
    turn = jax.random.randint(jax.random.fold_in(own, 2), (rows, 1), 0, top)
    return jnp.take_along_axis(grid, (jnp.arange(top)[None, :] + turn) % top, axis=1)


def portions_of(number_of, total, bound, skew, full):
    loads = [(1 << 20) // math.isqrt(standing ** skew) + 1 for standing in range(1, number_of + 1)]
    largest = bound if full else min(bound, max(-(-total // number_of), total * loads[0] // sum(loads)))
    least = 1 if total - largest >= number_of - 1 else 0
    counts, spare = [largest] + [least] * (number_of - 1), total - largest - least * (number_of - 1)
    while spare > 0:
        free = [i for i in range(1, number_of) if counts[i] < largest] or [i for i in range(1, number_of) if counts[i] < bound]
        mass, budget = sum([loads[i] for i in free]), spare
        for i in free:
            more = min(bound - counts[i], max(1, budget * loads[i] // mass), spare)
            counts[i] = counts[i] + more
            spare = spare - more
    return np.array(counts)


def centred(key, extent, width, bound, pieces=(), held_as=jnp.bfloat16):
    entries = jax.random.normal(key, extent, jnp.float32) * width
    if len(pieces) > 0:
        entries = steps_of(key, extent, pieces, -0.22, 0.18) * entries
    return jnp.clip(entries, min=-bound, max=bound).astype(held_as)


def heavy_noise(own_key, extent, width, limit, pieces, heavy, held_as=jnp.bfloat16):
    result = width * jax.random.normal(own_key, extent, jnp.float32)
    if pieces:
        result = result * steps_of(own_key, extent, pieces, -0.22, 0.18)
    return jnp.clip(with_spikes(result, jax.random.fold_in(own_key, 3), *heavy), -limit, limit).astype(held_as)


def setup_inputs(seed: int = 0) -> dict:
    splits = jax.random.split(jax.random.key(seed), 13)
    resid = centred(splits[0], (SEQUENCE_TOKENS, D), 1.0, 6.0, ((0, 8),))
    cotangent = heavy_noise(splits[1], (SEQUENCE_TOKENS, D), 0.1, 0.59765625, ((0, 8),), (0, 1, 8, 2.0))
    routes_keys = jax.random.split(jax.random.fold_in(splits[2], 1), SEQUENCE_TOKENS // TOK_DEV)
    routes_turns = jax.random.permutation(jax.random.fold_in(splits[2], 3), SEQUENCE_TOKENS // TOK_DEV)
    routes = jax.vmap(lambda own, number: shared_out(jax.random.fold_in(splits[2], 2), own, number, TOK_DEV, EXPERTS, TOP, CAP, 2))(routes_keys, routes_turns).reshape((SEQUENCE_TOKENS, TOP))
    route_weight = jnp.clip(jnp.exp(math.log(2.2) - 1.9924301 * jax.random.uniform(splits[3], (SEQUENCE_TOKENS, TOP), jnp.float32) ** steps_of(splits[3], (SEQUENCE_TOKENS, TOP), ((0, 8),), -0.2, 0.2)), 0.3, 2.2)
    w_gate = centred(splits[4], (EXPERTS, D, FE), D ** -0.5, 0.125, ((0, 8), (2, 4)))
    w_up = centred(splits[5], (EXPERTS, D, FE), D ** -0.5, 0.125, ((0, 8), (2, 4)))
    w_down = centred(splits[6], (EXPERTS, FE, D), FE ** -0.5, 0.1875, ((0, 8), (1, 4)))
    out_proj = centred(splits[7], (D, STATE_CHANNELS), STATE_CHANNELS ** -0.5, 0.109375, ((1, 4),))
    gate_pre = centred(splits[8], (SEQUENCE_TOKENS, STATE_CHANNELS), 1.5, 8.0, ((0, 8), (1, 4)))
    log_decay = draw_log_decay(jax.random.fold_in(splits[12], 71), 0)
    state_before = centred(splits[10], (SEQUENCE_TOKENS, STATE_CHANNELS), 1.0, 6.0, ((0, 8), (1, 4)), jnp.float32)
    step_input = centred(splits[11], (SEQUENCE_TOKENS, STATE_CHANNELS), 1.0, 6.0, ((0, 8), (1, 4)))
    return {"resid": resid, "cotangent": cotangent, "routes": routes, "route_weight": route_weight, "w_gate": w_gate, "w_up": w_up, "w_down": w_down, "out_proj": out_proj, "gate_pre": gate_pre, "log_decay": log_decay, "state_before": state_before, "step_input": step_input}


def slot_table(routes, route_weight):
    flat_ids = routes.reshape(N_SP, TOK_DEV * TOP)
    onehot = (flat_ids[:, :, None] == jnp.arange(EXPERTS, dtype=jnp.int32)[None, None, :]).astype(jnp.int32)
    ranking = lax.optimization_barrier(jnp.sum((jnp.cumsum(onehot, axis=1) - onehot) * onehot, axis=2)).reshape(-1)
    expert_ids = routes.reshape(-1)
    token_ids = jnp.arange(SEQUENCE_TOKENS * TOP, dtype=jnp.int32) // TOP
    block_ids = token_ids // TOK_DEV
    slot_token = jnp.full((EXPERTS, N_SP, CAP), SEQUENCE_TOKENS, jnp.int32).at[expert_ids, block_ids, ranking].set(token_ids)
    slot_weight = jnp.zeros((EXPERTS, N_SP, CAP), jnp.float32).at[expert_ids, block_ids, ranking].set(route_weight.reshape(-1))
    return (slot_token, slot_weight)

def one_expert(operands):
    token_ids, weights, resid_pad, cot_pad, gate_w, up_w, down_w = operands
    in_rows = resid_pad[token_ids]
    cot_rows = (weights[:, None] * cot_pad[token_ids].astype(jnp.float32)).astype(jnp.bfloat16)
    gate_act = jnp.dot(in_rows, gate_w, preferred_element_type=jnp.float32)
    up_act = jnp.dot(in_rows, up_w, preferred_element_type=jnp.float32)
    sigmoid_a = jax.nn.sigmoid(gate_act)
    hidden = (jax.nn.silu(gate_act) * up_act).astype(jnp.bfloat16)
    grad_down = jnp.dot(hidden.T, cot_rows, preferred_element_type=jnp.float32)
    d_hidden = jnp.dot(cot_rows, down_w.T, preferred_element_type=jnp.float32)
    slope = sigmoid_a * (1.0 + gate_act * (1.0 - sigmoid_a))
    d_gate_act = (d_hidden * up_act * slope).astype(jnp.bfloat16)
    d_up_act = (d_hidden * jax.nn.silu(gate_act)).astype(jnp.bfloat16)
    grad_gate = jnp.dot(in_rows.T, d_gate_act, preferred_element_type=jnp.float32)
    grad_up = jnp.dot(in_rows.T, d_up_act, preferred_element_type=jnp.float32)
    row_count = in_rows.shape[0]
    group = FE // N_TP
    parts = jnp.einsum('rpf,dpf->prd', d_gate_act.reshape(row_count, N_TP, group).astype(jnp.float32), gate_w.reshape(D, N_TP, group).astype(jnp.float32))
    parts = parts + jnp.einsum('rpf,dpf->prd', d_up_act.reshape(row_count, N_TP, group).astype(jnp.float32), up_w.reshape(D, N_TP, group).astype(jnp.float32))
    rounded = lax.optimization_barrier(parts.astype(jnp.bfloat16))
    expert_grad = lax.optimization_barrier(jnp.sum(rounded.astype(jnp.float32), axis=0)).astype(jnp.bfloat16)
    return (grad_gate, grad_up, grad_down, expert_grad)

def reverse_link(former, latter):
    return (former[0] * latter[0], latter[0] * former[1] + latter[1])

def reference(resid, cotangent, routes, route_weight, w_gate, w_up, w_down, out_proj, gate_pre, log_decay, state_before, step_input):
    slot_token, slot_weight = slot_table(routes, route_weight)
    resid_pad = jnp.concatenate([resid, jnp.zeros((1, D), jnp.bfloat16)], axis=0)
    cot_pad = jnp.concatenate([cotangent, jnp.zeros((1, D), jnp.bfloat16)], axis=0)

    def per_expert(operands):
        token_ids, weights, gate_w, up_w, down_w = operands
        return one_expert((token_ids.reshape(-1), weights.reshape(-1), resid_pad, cot_pad, gate_w, up_w, down_w))
    grad_gate, grad_up, grad_down, expert_grad = lax.map(per_expert, (slot_token, slot_weight, w_gate, w_up, w_down))
    routed = jnp.zeros((SEQUENCE_TOKENS + 1, D), jnp.float32).at[slot_token.reshape(-1)].add(expert_grad.reshape(-1, D).astype(jnp.float32))[:SEQUENCE_TOKENS]
    resid_grad = (cotangent.astype(jnp.float32) + routed).astype(jnp.bfloat16)
    decays = jnp.exp(log_decay)
    states = decays * state_before + step_input.astype(jnp.float32)
    gelu_val, gelu_back = jax.vjp(jax.nn.gelu, gate_pre.astype(jnp.float32))
    mixed = (gelu_val * states).astype(jnp.bfloat16)
    d_mixed = jnp.dot(resid_grad, out_proj, preferred_element_type=jnp.float32)
    grad_gate_pre = gelu_back(d_mixed * states)[0].astype(jnp.bfloat16)
    grad_proj = jnp.dot(resid_grad.T, mixed, preferred_element_type=jnp.float32)
    direct = d_mixed * gelu_val
    following = jnp.concatenate([decays[1:], jnp.zeros((1, STATE_CHANNELS), jnp.float32)], axis=0)
    scanned = lax.associative_scan(reverse_link, (jnp.flip(following, 0), jnp.flip(direct, 0)), axis=0)
    grad_step_input = jnp.flip(scanned[1], 0)
    grad_log_decay = grad_step_input * decays * state_before
    return (grad_gate, grad_up, grad_down, grad_proj, grad_gate_pre, grad_step_input, grad_log_decay)
```

```python
import functools

import jax
import jax.numpy as jnp
from jax import lax
from jax.sharding import PartitionSpec as P


from jax.experimental import pallas as pl
from jax.experimental.pallas import tpu as pltpu

MESH_IDS = pl.DeviceIdType.MESH
SUBLANES = 8
CUBIC = 0.044715
TANH_SCALE = 0.7978845608028654


def recurrence_kernel(
    dm_ref, pre_ref, ld_ref, sb_ref, si_ref, ggp_ref, loc_ref, prod_ref, edge_ref, carry
):
    rows, channels = dm_ref.shape

    @pl.when(pl.program_id(0) == 0)
    def _():
        carry[0:1, :] = jnp.zeros((1, channels), jnp.float32)
        carry[1:2, :] = jnp.ones((1, channels), jnp.float32)

    row = lax.broadcasted_iota(jnp.int32, (SUBLANES, channels), 0)

    def ahead(x, k, fill):
        return jnp.where(row < SUBLANES - k, pltpu.roll(x, SUBLANES - k, 0), fill)

    def pair(j, state):
        shift_in, scale_in = state
        start = pl.multiple_of(rows - 2 * SUBLANES * (j + 1), 2 * SUBLANES)
        both = pl.ds(start, 2 * SUBLANES)
        pre = pre_ref[both, :].astype(jnp.float32)
        step_in = si_ref[both, :].astype(jnp.float32)
        dm = dm_ref[both, :]
        decay = jnp.exp(ld_ref[both, :])
        state_val = decay * sb_ref[both, :] + step_in
        square = pre * pre
        tanh = jnp.tanh(TANH_SCALE * (pre + CUBIC * square * pre))
        half = 0.5 * (1.0 + tanh)
        slope = half + 0.5 * pre * (1.0 - tanh * tanh) * (
            TANH_SCALE * (1.0 + 3.0 * CUBIC * square)
        )
        direct = dm * (pre * half)
        ggp_ref[both, :] = (dm * state_val * slope).astype(jnp.bfloat16)
        for part in (1, 0):
            lo = part * SUBLANES
            own = direct[lo : lo + SUBLANES]
            scale = decay[lo : lo + SUBLANES]
            shift = scale * own
            for k in (1, 2, 4):
                shift = shift + scale * ahead(shift, k, 0.0)
                scale = scale * ahead(scale, k, 1.0)
            shift = shift + scale * shift_in
            scale = scale * scale_in
            loc_ref[pl.ds(start + lo, SUBLANES), :] = own + ahead(shift, 1, shift_in)
            prod_ref[pl.ds(start + lo, SUBLANES), :] = ahead(scale, 1, scale_in)
            shift_in = shift[0:1]
            scale_in = scale[0:1]
        return (shift_in, scale_in)

    shift_in, scale_in = lax.fori_loop(
        0, rows // (2 * SUBLANES), pair, (carry[0:1, :], carry[1:2, :])
    )
    carry[0:1, :] = shift_in
    carry[1:2, :] = scale_in
    edge_ref[...] = jnp.where(row == 0, scale_in, shift_in)


def local_recurrence(d_mixed, gate_pre, log_decay, state_before, step_input):
    tokens, channels = d_mixed.shape
    steps = 1
    while tokens % (2 * steps * 2 * SUBLANES) == 0 and steps < 4:
        steps = 2 * steps
    block = pl.BlockSpec((tokens // steps, channels), lambda i: (steps - 1 - i, 0))
    wide = jax.ShapeDtypeStruct((tokens, channels), jnp.float32)
    return pl.pallas_call(
        recurrence_kernel,
        grid=(steps,),
        in_specs=[block] * 5,
        out_specs=[block] * 3 + [pl.BlockSpec((SUBLANES, channels), lambda i: (0, 0))],
        out_shape=[
            jax.ShapeDtypeStruct((tokens, channels), jnp.bfloat16),
            wide,
            wide,
            jax.ShapeDtypeStruct((SUBLANES, channels), jnp.float32),
        ],
        scratch_shapes=[pltpu.VMEM((SUBLANES, channels), jnp.float32)],
        compiler_params=pltpu.CompilerParams(dimension_semantics=("arbitrary",)),
        cost_estimate=pl.CostEstimate(
            flops=60 * tokens * channels,
            bytes_accessed=28 * tokens * channels,
            transcendentals=2 * tokens * channels,
        ),
        name="local_recurrence",
    )(d_mixed, gate_pre, log_decay, state_before, step_input)


def carry_kernel(count, edge_ref, out_ref, held, send_sem, recv_sem):
    place = lax.axis_index("sp")
    barrier = pltpu.get_barrier_semaphore()
    for k in range(1, count):
        pl.semaphore_signal(
            barrier, inc=1, device_id={"sp": lax.rem(place + k, count)}, device_id_type=MESH_IDS
        )
    pl.semaphore_wait(barrier, count - 1)
    sends = []
    for k in range(1, count):
        copy = pltpu.make_async_remote_copy(
            src_ref=edge_ref,
            dst_ref=held.at[k],
            send_sem=send_sem.at[k],
            recv_sem=recv_sem.at[k],
            device_id={"sp": lax.rem(place + count - k, count)},
            device_id_type=MESH_IDS,
        )
        copy.start()
        sends.append(copy)
    for copy in sends:
        copy.wait()
    value = jnp.zeros((1, edge_ref.shape[1]), jnp.float32)
    for k in range(count - 1, 0, -1):
        turn = held[k, 0:1, :] * value + held[k, 1:2, :]
        value = jnp.where(place + k < count, turn, value)
    out_ref[...] = jnp.broadcast_to(value, out_ref.shape)


def carried_in(edge):
    count = lax.axis_size("sp")
    channels = edge.shape[1]
    arriving = pl.pallas_call(
        functools.partial(carry_kernel, count),
        out_shape=jax.ShapeDtypeStruct((SUBLANES, channels), jnp.float32),
        in_specs=[pl.BlockSpec(memory_space=pltpu.VMEM)],
        out_specs=pl.BlockSpec(memory_space=pltpu.VMEM),
        scratch_shapes=[
            pltpu.VMEM((count, SUBLANES, channels), jnp.float32),
            pltpu.SemaphoreType.DMA((count,)),
            pltpu.SemaphoreType.DMA((count,)),
        ],
        compiler_params=pltpu.CompilerParams(collective_id=1, has_side_effects=True),
        cost_estimate=pl.CostEstimate(
            flops=20000, bytes_accessed=8000000, transcendentals=0
        ),
        name="carry_exchange",
    )(edge)
    return arriving[0:1]


def expert_work(in_rows, cot_rows, gate_w, up_w, down_w):
    gate_act = jnp.dot(in_rows, gate_w, preferred_element_type=jnp.float32)
    up_act = jnp.dot(in_rows, up_w, preferred_element_type=jnp.float32)
    sigmoid_a = jax.nn.sigmoid(gate_act)
    hidden = (jax.nn.silu(gate_act) * up_act).astype(jnp.bfloat16)
    grad_down = lax.dot_general(
        hidden, cot_rows, (((0,), (0,)), ((), ())), preferred_element_type=jnp.float32
    )
    d_hidden = lax.dot_general(
        cot_rows, down_w, (((1,), (1,)), ((), ())), preferred_element_type=jnp.float32
    )
    slope = sigmoid_a * (1.0 + gate_act * (1.0 - sigmoid_a))
    d_gate_act = (d_hidden * up_act * slope).astype(jnp.bfloat16)
    d_up_act = (d_hidden * jax.nn.silu(gate_act)).astype(jnp.bfloat16)
    grad_gate = lax.dot_general(
        in_rows, d_gate_act, (((0,), (0,)), ((), ())), preferred_element_type=jnp.float32
    )
    grad_up = lax.dot_general(
        in_rows, d_up_act, (((0,), (0,)), ((), ())), preferred_element_type=jnp.float32
    )
    partial_value = lax.dot_general(
        d_gate_act, gate_w, (((1,), (1,)), ((), ())), preferred_element_type=jnp.float32
    )
    partial_value = partial_value + lax.dot_general(
        d_up_act, up_w, (((1,), (1,)), ((), ())), preferred_element_type=jnp.float32
    )
    rounded = lax.optimization_barrier(partial_value.astype(jnp.bfloat16))
    return (grad_gate[None], grad_up[None], grad_down[None], rounded.astype(jnp.float32))


def gather_slots(resid_part, cot_part, slot_token, slot_weight, groups, capacity):
    col_width = resid_part.shape[1]
    resid_pad = jnp.concatenate([resid_part, jnp.zeros((1, col_width), jnp.bfloat16)], axis=0)
    cot_pad = jnp.concatenate([cot_part, jnp.zeros((1, col_width), jnp.bfloat16)], axis=0)
    send_rows = resid_pad[slot_token].reshape(groups, capacity, col_width)
    send_cot = (slot_weight[:, None] * cot_pad[slot_token].astype(jnp.float32)).astype(jnp.bfloat16)
    return (send_rows, send_cot.reshape(groups, capacity, col_width))


def combine_slots(returned, cot_part, slot_ids, tok_rows, top_count):
    col_width = returned.shape[2]
    flat_back = returned.reshape(-1, col_width)
    routed = jnp.sum(
        flat_back[slot_ids].astype(jnp.float32).reshape(tok_rows, top_count, col_width), axis=1
    )
    return (cot_part.astype(jnp.float32) + routed).astype(jnp.bfloat16)


def on_device(
    resid,
    cotangent,
    routes,
    route_weight,
    w_gate,
    w_up,
    w_down,
    out_proj,
    gate_pre,
    log_decay,
    state_before,
    step_input,
):
    tok_rows, model_width = resid.shape
    top_count = routes.shape[1]
    groups = lax.axis_size("sp")
    capacity = 2 * tok_rows * top_count // groups
    flat_ids = routes.reshape(-1)
    onehot = (flat_ids[:, None] == jnp.arange(groups, dtype=jnp.int32)[None, :]).astype(jnp.int32)
    ranking = jnp.sum((jnp.cumsum(onehot, axis=0) - onehot) * onehot, axis=1)
    slot_ids = flat_ids * capacity + ranking
    member = slot_ids[None, :] == jnp.arange(groups * capacity, dtype=jnp.int32)[:, None]
    token_ids = jnp.arange(tok_rows * top_count, dtype=jnp.int32) // top_count
    filled = jnp.any(member, axis=1)
    slot_token = jnp.where(
        filled, jnp.sum(jnp.where(member, token_ids[None, :], 0), axis=1), tok_rows
    )
    slot_weight = jnp.sum(jnp.where(member, route_weight.reshape(-1)[None, :], 0.0), axis=1)
    col_width = model_width // lax.axis_size("tp")
    col_start = lax.axis_index("tp") * col_width
    cot_part = lax.dynamic_slice_in_dim(cotangent, col_start, col_width, 1)
    resid_part = lax.dynamic_slice_in_dim(resid, col_start, col_width, 1)
    send_rows, send_cot = gather_slots(
        resid_part, cot_part, slot_token, slot_weight, groups, capacity
    )
    got_rows, got_cot = (
        lax.all_to_all(send_rows, "sp", split_axis=0, concat_axis=0, tiled=True),
        lax.all_to_all(send_cot, "sp", split_axis=0, concat_axis=0, tiled=True),
    )
    full_rows, full_cot = (
        lax.all_gather(got_rows, "tp", axis=2, tiled=True),
        lax.all_gather(got_cot, "tp", axis=2, tiled=True),
    )
    grad_gate, grad_up, grad_down, partial_value = expert_work(
        full_rows.reshape(-1, model_width),
        full_cot.reshape(-1, model_width),
        w_gate[0],
        w_up[0],
        w_down[0],
    )
    summed = lax.psum_scatter(
        partial_value.reshape(groups, capacity, model_width).astype(jnp.bfloat16),
        "tp",
        scatter_dimension=2,
        tiled=True,
    )
    returned = lax.all_to_all(summed, "sp", split_axis=0, concat_axis=0, tiled=True)
    part_grad = combine_slots(returned, cot_part, slot_ids, tok_rows, top_count)
    resid_grad = lax.all_gather(part_grad, "tp", axis=1, tiled=True)
    decays = jnp.exp(log_decay)
    states = decays * state_before + step_input.astype(jnp.float32)
    mixed = (jax.nn.gelu(gate_pre.astype(jnp.float32)) * states).astype(jnp.bfloat16)
    d_mixed = jnp.dot(resid_grad, out_proj, preferred_element_type=jnp.float32)
    grad_proj = lax.psum_scatter(
        lax.dot_general(
            resid_grad, mixed, (((0,), (0,)), ((), ())), preferred_element_type=jnp.float32
        ).astype(jnp.bfloat16),
        "sp",
        scatter_dimension=0,
        tiled=True,
    ).astype(jnp.float32)
    grad_gate_pre, local_vals, products, edge = local_recurrence(
        d_mixed, gate_pre, log_decay, state_before, step_input
    )
    arriving = carried_in(edge)
    grad_step_input = local_vals + products * arriving
    grad_log_decay = grad_step_input * decays * state_before
    return (
        grad_gate,
        grad_up,
        grad_down,
        grad_proj,
        grad_gate_pre,
        grad_step_input,
        grad_log_decay,
    )


def solution(mesh):
    return jax.shard_map(
        on_device,
        mesh=mesh,
        in_specs=(
            P("sp", None),
            P("sp", None),
            P("sp", None),
            P("sp", None),
            P("sp", None, "tp"),
            P("sp", None, "tp"),
            P("sp", "tp", None),
            P(None, "tp"),
            P("sp", "tp"),
            P("sp", "tp"),
            P("sp", "tp"),
            P("sp", "tp"),
        ),
        out_specs=(
            P("sp", None, "tp"),
            P("sp", None, "tp"),
            P("sp", "tp", None),
            P("sp", "tp"),
            P("sp", "tp"),
            P("sp", "tp"),
            P("sp", "tp"),
        ),
        check_vma=False,
    )
```

```python
import functools

import jax
import jax.numpy as jnp
from jax import lax
from jax.sharding import PartitionSpec as P


from jax.experimental import pallas as pl
from jax.experimental.pallas import tpu as pltpu

MESH_IDS = pl.DeviceIdType.MESH
SUBLANES = 8
CUBIC = 0.044715
TANH_SCALE = 0.7978845608028654


def recurrence_kernel(
    dm_ref, pre_ref, ld_ref, sb_ref, si_ref, ggp_ref, loc_ref, prod_ref, edge_ref, carry
):
    rows, channels = dm_ref.shape

    @pl.when(pl.program_id(0) == 0)
    def _():
        carry[0:1, :] = jnp.zeros((1, channels), jnp.float32)
        carry[1:2, :] = jnp.ones((1, channels), jnp.float32)

    row = lax.broadcasted_iota(jnp.int32, (SUBLANES, channels), 0)

    def ahead(x, k, fill):
        return jnp.where(row < SUBLANES - k, pltpu.roll(x, SUBLANES - k, 0), fill)

    def pair(j, state):
        shift_in, scale_in = state
        start = pl.multiple_of(rows - 2 * SUBLANES * (j + 1), 2 * SUBLANES)
        both = pl.ds(start, 2 * SUBLANES)
        pre = pre_ref[both, :].astype(jnp.float32)
        step_in = si_ref[both, :].astype(jnp.float32)
        dm = dm_ref[both, :]
        decay = jnp.exp(ld_ref[both, :])
        state_val = decay * sb_ref[both, :] + step_in
        square = pre * pre
        tanh = jnp.tanh(TANH_SCALE * (pre + CUBIC * square * pre))
        half = 0.5 * (1.0 + tanh)
        slope = half + 0.5 * pre * (1.0 - tanh * tanh) * (
            TANH_SCALE * (1.0 + 3.0 * CUBIC * square)
        )
        direct = dm * (pre * half)
        ggp_ref[both, :] = (dm * state_val * slope).astype(jnp.bfloat16)
        for part in (1, 0):
            lo = part * SUBLANES
            own = direct[lo : lo + SUBLANES]
            scale = decay[lo : lo + SUBLANES]
            shift = scale * own
            for k in (1, 2, 4):
                shift = shift + scale * ahead(shift, k, 0.0)
                scale = scale * ahead(scale, k, 1.0)
            shift = shift + scale * shift_in
            scale = scale * scale_in
            loc_ref[pl.ds(start + lo, SUBLANES), :] = own + ahead(shift, 1, shift_in)
            prod_ref[pl.ds(start + lo, SUBLANES), :] = ahead(scale, 1, scale_in)
            shift_in = shift[0:1]
            scale_in = scale[0:1]
        return (shift_in, scale_in)

    shift_in, scale_in = lax.fori_loop(
        0, rows // (2 * SUBLANES), pair, (carry[0:1, :], carry[1:2, :])
    )
    carry[0:1, :] = shift_in
    carry[1:2, :] = scale_in
    edge_ref[...] = jnp.where(row == 0, scale_in, shift_in)


def local_recurrence(d_mixed, gate_pre, log_decay, state_before, step_input):
    tokens, channels = d_mixed.shape
    steps = 1
    while tokens % (2 * steps * 2 * SUBLANES) == 0 and steps < 4:
        steps = 2 * steps
    block = pl.BlockSpec((tokens // steps, channels), lambda i: (steps - 1 - i, 0))
    wide = jax.ShapeDtypeStruct((tokens, channels), jnp.float32)
    return pl.pallas_call(
        recurrence_kernel,
        grid=(steps,),
        in_specs=[block] * 5,
        out_specs=[block] * 3 + [pl.BlockSpec((SUBLANES, channels), lambda i: (0, 0))],
        out_shape=[
            jax.ShapeDtypeStruct((tokens, channels), jnp.bfloat16),
            wide,
            wide,
            jax.ShapeDtypeStruct((SUBLANES, channels), jnp.float32),
        ],
        scratch_shapes=[pltpu.VMEM((SUBLANES, channels), jnp.float32)],
        compiler_params=pltpu.CompilerParams(dimension_semantics=("arbitrary",)),
        cost_estimate=pl.CostEstimate(
            flops=60 * tokens * channels,
            bytes_accessed=28 * tokens * channels,
            transcendentals=2 * tokens * channels,
        ),
        name="local_recurrence",
    )(d_mixed, gate_pre, log_decay, state_before, step_input)


def carry_kernel(count, edge_ref, out_ref, held, send_sem, recv_sem):
    place = lax.axis_index("sp")
    barrier = pltpu.get_barrier_semaphore()
    for k in range(1, count):
        pl.semaphore_signal(
            barrier, inc=1, device_id={"sp": lax.rem(place + k, count)}, device_id_type=MESH_IDS
        )
    pl.semaphore_wait(barrier, count - 1)
    sends = []
    for k in range(1, count):
        copy = pltpu.make_async_remote_copy(
            src_ref=edge_ref,
            dst_ref=held.at[k],
            send_sem=send_sem.at[k],
            recv_sem=recv_sem.at[k],
            device_id={"sp": lax.rem(place + count - k, count)},
            device_id_type=MESH_IDS,
        )
        copy.start()
        sends.append(copy)
    for copy in sends:
        copy.wait()
    value = jnp.zeros((1, edge_ref.shape[1]), jnp.float32)
    for k in range(count - 1, 0, -1):
        turn = held[k, 0:1, :] * value + held[k, 1:2, :]
        value = jnp.where(place + k < count, turn, value)
    out_ref[...] = jnp.broadcast_to(value, out_ref.shape)


def carried_in(edge):
    count = lax.axis_size("sp")
    channels = edge.shape[1]
    arriving = pl.pallas_call(
        functools.partial(carry_kernel, count),
        out_shape=jax.ShapeDtypeStruct((SUBLANES, channels), jnp.float32),
        in_specs=[pl.BlockSpec(memory_space=pltpu.VMEM)],
        out_specs=pl.BlockSpec(memory_space=pltpu.VMEM),
        scratch_shapes=[
            pltpu.VMEM((count, SUBLANES, channels), jnp.float32),
            pltpu.SemaphoreType.DMA((count,)),
            pltpu.SemaphoreType.DMA((count,)),
        ],
        compiler_params=pltpu.CompilerParams(collective_id=1, has_side_effects=True),
        cost_estimate=pl.CostEstimate(
            flops=20000, bytes_accessed=8000000, transcendentals=0
        ),
        name="carry_exchange",
    )(edge)
    return arriving[0:1]


def mixed_kernel(pre_ref, ld_ref, sb_ref, si_ref, out_ref):
    pre = pre_ref[...].astype(jnp.float32)
    half = 0.5 * (1.0 + jnp.tanh(TANH_SCALE * (pre + CUBIC * pre * pre * pre)))
    states = jnp.exp(ld_ref[...]) * sb_ref[...] + si_ref[...].astype(jnp.float32)
    out_ref[...] = (pre * half * states).astype(jnp.bfloat16)


def mixed_of(gate_pre, log_decay, state_before, step_input):
    tokens, channels = gate_pre.shape
    steps = tokens // 32 if tokens % 32 == 0 else 1
    block = pl.BlockSpec((tokens // steps, channels), lambda i: (i, 0))
    return pl.pallas_call(
        mixed_kernel,
        grid=(steps,),
        in_specs=[block] * 4,
        out_specs=block,
        out_shape=jax.ShapeDtypeStruct((tokens, channels), jnp.bfloat16),
        compiler_params=pltpu.CompilerParams(dimension_semantics=("arbitrary",)),
        cost_estimate=pl.CostEstimate(
            flops=20 * tokens * channels,
            bytes_accessed=14 * tokens * channels,
            transcendentals=2 * tokens * channels,
        ),
        name="mixed",
    )(gate_pre, log_decay, state_before, step_input)


def transposed_dot(left, right):
    return lax.dot_general(
        left, right, (((0,), (0,)), ((), ())), preferred_element_type=jnp.float32
    )


def dot_transposed(left, right):
    return lax.dot_general(
        left, right, (((1,), (1,)), ((), ())), preferred_element_type=jnp.float32
    )


def expert_grad_of(in_rows, cot_rows, gate_w, up_w, down_w):
    gate_act = jnp.dot(in_rows, gate_w, preferred_element_type=jnp.float32)
    up_act = jnp.dot(in_rows, up_w, preferred_element_type=jnp.float32)
    sigmoid_a = jax.nn.sigmoid(gate_act)
    silu = gate_act * sigmoid_a
    hidden = (silu * up_act).astype(jnp.bfloat16)
    d_hidden = dot_transposed(cot_rows, down_w)
    slope = sigmoid_a * (1.0 + gate_act * (1.0 - sigmoid_a))
    d_gate_act = (d_hidden * up_act * slope).astype(jnp.bfloat16)
    d_up_act = (d_hidden * silu).astype(jnp.bfloat16)
    partial_value = dot_transposed(d_gate_act, gate_w) + dot_transposed(d_up_act, up_w)
    return partial_value.astype(jnp.bfloat16), hidden, d_gate_act, d_up_act


def on_device(
    resid,
    cotangent,
    routes,
    route_weight,
    w_gate,
    w_up,
    w_down,
    out_proj,
    gate_pre,
    log_decay,
    state_before,
    step_input,
):
    tok_rows, model_width = resid.shape
    top_count = routes.shape[1]
    groups = lax.axis_size("sp")
    capacity = 2 * tok_rows * top_count // groups
    pieces = 2
    part_rows = capacity // pieces
    flat_ids = routes.reshape(-1)
    onehot = (flat_ids[:, None] == jnp.arange(groups, dtype=jnp.int32)[None, :]).astype(jnp.int32)
    ranking = jnp.sum((jnp.cumsum(onehot, axis=0) - onehot) * onehot, axis=1)
    slot_ids = (flat_ids * capacity + ranking).reshape(tok_rows, top_count)
    col_width = model_width // lax.axis_size("tp")
    col_start = lax.axis_index("tp") * col_width
    cot_part = lax.dynamic_slice_in_dim(cotangent, col_start, col_width, 1)
    resid_part = lax.dynamic_slice_in_dim(resid, col_start, col_width, 1)
    group_base = jnp.arange(groups, dtype=jnp.int32)[:, None] * capacity
    sends = []
    members = []
    for piece in range(pieces):
        slots = group_base + piece * part_rows + jnp.arange(part_rows, dtype=jnp.int32)[None, :]
        slots = slots.reshape(-1)
        match = [slots[:, None] == slot_ids[None, :, k] for k in range(top_count)]
        weight = sum(
            jnp.sum(jnp.where(m, route_weight[None, :, k], 0.0), axis=1)
            for k, m in enumerate(match)
        )
        member = functools.reduce(jnp.logical_or, match).astype(jnp.bfloat16)
        members.append(member)
        rows = jnp.dot(member, resid_part, preferred_element_type=jnp.float32)
        cots = jnp.dot(member, cot_part, preferred_element_type=jnp.float32)
        sends.append(
            (
                rows.astype(jnp.bfloat16).reshape(groups, part_rows, col_width),
                (weight[:, None] * cots)
                .astype(jnp.bfloat16)
                .reshape(groups, part_rows, col_width),
            )
        )

    def exchange(x):
        return lax.all_to_all(x, "sp", split_axis=0, concat_axis=0, tiled=True)

    def widen(x):
        return lax.all_gather(x, "tp", axis=2, tiled=True)

    got = []
    token = None
    for rows, cots in sends:
        for x in (rows, cots):
            if token is not None:
                x, token = lax.optimization_barrier((x, token))
            token = exchange(x)
            got.append(token)
    full = [widen(x) for x in got]
    full[0], full[1], _ = lax.optimization_barrier((full[0], full[1], got[-1]))
    acts = []
    summed = []
    for piece in range(pieces):
        in_rows = full[2 * piece].reshape(-1, model_width)
        cot_rows = full[2 * piece + 1].reshape(-1, model_width)
        partial_value, hidden, d_gate_act, d_up_act = expert_grad_of(
            in_rows, cot_rows, w_gate[0], w_up[0], w_down[0]
        )
        acts.append((in_rows, cot_rows, hidden, d_gate_act, d_up_act))
        summed.append(
            lax.psum_scatter(
                partial_value.reshape(groups, part_rows, model_width),
                "tp",
                scatter_dimension=2,
                tiled=True,
            )
        )
    grad_gate = sum(transposed_dot(i, g) for i, c, h, g, u in acts)
    grad_up = sum(transposed_dot(i, u) for i, c, h, g, u in acts)
    grad_down = sum(transposed_dot(h, c) for i, c, h, g, u in acts)
    mixed = mixed_of(gate_pre, log_decay, state_before, step_input)
    summed[-1], grad_gate, grad_up, grad_down, mixed = lax.optimization_barrier(
        (summed[-1], grad_gate, grad_up, grad_down, mixed)
    )
    returned = [exchange(x) for x in summed]
    routed = sum(
        transposed_dot(member, back.reshape(-1, col_width))
        for member, back in zip(members, returned)
    )
    part_grad = (cot_part.astype(jnp.float32) + routed).astype(jnp.bfloat16)
    resid_grad = lax.all_gather(part_grad, "tp", axis=1, tiled=True)
    decays = jnp.exp(log_decay)
    grad_proj = lax.psum_scatter(
        transposed_dot(resid_grad, mixed).astype(jnp.bfloat16),
        "sp",
        scatter_dimension=0,
        tiled=True,
    ).astype(jnp.float32)
    d_mixed = jnp.dot(resid_grad, out_proj, preferred_element_type=jnp.float32)
    grad_gate_pre, local_vals, products, edge = local_recurrence(
        d_mixed, gate_pre, log_decay, state_before, step_input
    )
    arriving = carried_in(edge)
    grad_step_input = local_vals + products * arriving
    grad_log_decay = grad_step_input * decays * state_before
    return (
        grad_gate[None],
        grad_up[None],
        grad_down[None],
        grad_proj,
        grad_gate_pre,
        grad_step_input,
        grad_log_decay,
    )


def solution(mesh):
    return jax.shard_map(
        on_device,
        mesh=mesh,
        in_specs=(
            P("sp", None),
            P("sp", None),
            P("sp", None),
            P("sp", None),
            P("sp", None, "tp"),
            P("sp", None, "tp"),
            P("sp", "tp", None),
            P(None, "tp"),
            P("sp", "tp"),
            P("sp", "tp"),
            P("sp", "tp"),
            P("sp", "tp"),
        ),
        out_specs=(
            P("sp", None, "tp"),
            P("sp", None, "tp"),
            P("sp", "tp", None),
            P("sp", "tp"),
            P("sp", "tp"),
            P("sp", "tp"),
            P("sp", "tp"),
        ),
        check_vma=False,
    )
```
